32 devices in a mesh: grp: 2 (over y), sp: 4 (over z), tp: 4 (over x, core).
Axes of the slice: x: 2, y: 2, z: 4, core: 2. Of those that a mesh axis runs over, the one named last changes fastest.
Arguments:
- hidden_in: bfloat16 [2048, 2048], P(('grp', 'sp'), 'tp'), parts along dimension 0, may hold values from -40 to 40
- norm_gain: float32 [3, 2048], replicated, may hold values from 0.1 to 1.9
- query_weight: bfloat16 [3, 1024, 2048], P(None, 'tp'), may hold values from -6 to 6
- key_weight: bfloat16 [3, 1024, 2048], P(None, 'tp'), may hold values from -6 to 6
- value_weight: bfloat16 [3, 1024, 2048], P(None, 'tp'), may hold values from -0.125 to 0.125
- output_weight: bfloat16 [3, 1024, 2048], P(None, None, 'tp'), may hold values from -0.75 to 0.75
- offset_bias: float32 [3, 16, 15, 31], P(None, 'tp'), may hold values from -4 to 4
Outputs:
- hidden_out: bfloat16 [2048, 2048], P(('grp', 'sp'), 'tp'), parts along dimension 0
The draws below stay inside these ranges and needn't reach their ends.
There are 2 independent parts, one for each index of `grp`. The reference program is written for one: setup_inputs(seed, part) draws one part's arguments, and reference() takes and returns one part's arrays. A program takes and returns all parts, laid end to end along the dimension named above; an argument that names none is the same for every part. Nothing has to cross between parts.
All inputs are finite; a program needn't handle non-finite values.
Results may differ from the reference program's by a relative error of at most 0.028.
Values may be sent and summed in bfloat16 or wider, within the bound.
A program may use at most 64 MiB of HBM per device.

```python
import jax
import jax.numpy as jnp
import numpy as np
from jax import lax

D = 2048
HEADS = 16
HEAD_DIM = 64
GRID_W = 64
ROW_SPAN = 8
COL_SPAN = 16
LAYERS = 3
TOKENS = 1024


def query_draw(key):
    drawn = jax.random.normal(jax.random.fold_in(key, 101), (LAYERS, HEADS * HEAD_DIM, D), jnp.float32)
    return drawn * D ** (-0.5)


def draw_hidden_in(key, part):
    subkeys = jax.random.split(jax.random.fold_in(key, 505), 3)
    normal_part = jax.random.normal(subkeys[0], (TOKENS, D), jnp.float32)
    col_pos = jnp.arange(D, dtype=jnp.float32) / D
    col_scale = jnp.exp(jnp.log(4.0) * col_pos + jax.random.uniform(subkeys[1], (D,), jnp.float32, -0.6, 0.6))
    row_scale = jnp.exp(jax.random.uniform(subkeys[2], (TOKENS, 1), jnp.float32, -1.0, 1.0))
    values = normal_part * col_scale[None, :] * row_scale * 0.6
    return jnp.clip(values, -40.0, 40.0).astype(jnp.bfloat16)


def draw_query_weight(key, part):
    return jnp.clip(query_draw(key), -6.0, 6.0).astype(jnp.bfloat16)


def draw_key_weight(key, part):
    values = jax.random.normal(jax.random.fold_in(key, 202), (LAYERS, HEADS * HEAD_DIM, D), jnp.float32) * D ** (-0.5)
    return jnp.clip(values, -6.0, 6.0).astype(jnp.bfloat16)


def block_levels(rng, shape, shards, low, top_value):
    level = 1.0
    for axis_at, parts in shards:
        heights = jax.random.uniform(jax.random.fold_in(jax.random.fold_in(rng, 6), axis_at), (parts,), jnp.float32, low / len(shards), top_value / len(shards))
        level = level * jnp.repeat(jnp.exp(heights), shape[axis_at] // parts).reshape((-1,) + (1,) * (len(shape) - 1 - axis_at))
    return level


def scatter_about(key, dims, scale, most, cuts=(), held_as=jnp.bfloat16):
    gain = block_levels(key, dims, cuts, -0.22, 0.18) if cuts else 1.0
    values = jax.random.normal(key, dims, jnp.float32) * scale * gain
    return jnp.minimum(jnp.maximum(values, -most), most).astype(held_as)


def setup_inputs(seed: int = 0, part: int = 0) -> dict:
    key_of = jax.random.split(jax.random.key(seed), 8)
    part_keys = jax.random.split(jax.random.fold_in(key_of[7], part), 8)
    return {
        "hidden_in": draw_hidden_in(jax.random.fold_in(jax.random.fold_in(key_of[7], part), 71), part),
        "norm_gain": jnp.clip(1.0 + 0.18 * jax.random.normal(key_of[1], (LAYERS, D), jnp.float32), 0.1, 1.9),
        "query_weight": draw_query_weight(jax.random.fold_in(key_of[7], 71), part),
        "key_weight": draw_key_weight(jax.random.fold_in(key_of[7], 71), part),
        "value_weight": scatter_about(key_of[4], (LAYERS, HEADS * HEAD_DIM, D), D ** -0.5, 0.125, ((1, 4),)),
        "output_weight": scatter_about(key_of[5], (LAYERS, HEADS * HEAD_DIM, D), (HEADS * HEAD_DIM // 16) ** -0.5, 0.75, ((2, 4),)),
        "offset_bias": scatter_about(key_of[6], (LAYERS, HEADS, 2 * ROW_SPAN - 1, 2 * COL_SPAN - 1), 1.0, 4.0, ((1, 4),), jnp.float32),
    }


EPS = 1e-06
NEG = -1e+30
QBLOCK = 16

def column_tables():
    nblocks = GRID_W // QBLOCK
    key_span = QBLOCK + COL_SPAN
    block_start = np.clip(np.arange(nblocks) * QBLOCK - COL_SPAN // 2, 0, GRID_W - key_span)
    key_cols = block_start[:, None] + np.arange(key_span)[None, :]
    query_cols = np.arange(nblocks)[:, None] * QBLOCK + np.arange(QBLOCK)[None, :]
    window_cols = np.clip(query_cols - COL_SPAN // 2, 0, GRID_W - COL_SPAN)
    inside = (key_cols[:, None, :] >= window_cols[:, :, None]) & (key_cols[:, None, :] < window_cols[:, :, None] + COL_SPAN)
    col_offset = np.clip(key_cols[:, None, :] - query_cols[:, :, None], 1 - COL_SPAN, COL_SPAN - 1) + COL_SPAN - 1
    return (block_start, inside, col_offset)

def block_firsts():
    nblocks = GRID_W // QBLOCK
    key_span = QBLOCK + COL_SPAN
    return [min(max(block * QBLOCK - COL_SPAN // 2, 0), GRID_W - key_span) for block in range(nblocks)]

def bias_rows(bias_table, row_offset):
    block_start, inside, col_offset = column_tables()
    nblocks = block_start.shape[0]
    key_span = QBLOCK + COL_SPAN
    rows_n = row_offset.shape[0]
    heads_n = bias_table.shape[0]
    by_row = bias_table[:, row_offset]
    chosen = by_row[:, :, :, jnp.asarray(col_offset, dtype=jnp.int32)]
    chosen = chosen.transpose(1, 0, 3, 4, 2, 5)
    return chosen.reshape(rows_n, heads_n, nblocks, QBLOCK, ROW_SPAN * key_span)

def attend_rows(queries, key_rows, value_rows, bias):
    block_start, inside, col_offset = column_tables()
    nblocks = block_start.shape[0]
    key_span = QBLOCK + COL_SPAN
    rows_n, heads_n, head_size = (queries.shape[0], queries.shape[2], queries.shape[3])

    def pick_blocks(tensor):
        pieces = [tensor[:, :, first_col:first_col + key_span] for first_col in block_firsts()]
        return jnp.stack(pieces, axis=1).reshape(rows_n, nblocks, ROW_SPAN * key_span, heads_n, head_size)
    key_blocks = pick_blocks(key_rows).astype(jnp.float32)
    value_blocks = pick_blocks(value_rows).astype(jnp.float32)
    query_blocks = queries.reshape(rows_n, nblocks, QBLOCK, heads_n, head_size).astype(jnp.float32)
    scores = jnp.einsum('rcqhd,rckhd->rhcqk', query_blocks, key_blocks) * head_size ** (-0.5) + bias
    allowed = np.broadcast_to(inside[:, :, None, :], (nblocks, QBLOCK, ROW_SPAN, key_span))
    allowed = allowed.reshape(nblocks, QBLOCK, ROW_SPAN * key_span)
    scores = jnp.where(jnp.asarray(allowed)[None, None], scores, NEG)
    row_peak = lax.optimization_barrier(jnp.max(scores, axis=-1, keepdims=True))
    lifted = jnp.exp(scores - row_peak)
    weights = (lifted / lax.optimization_barrier(jnp.sum(lifted, axis=-1, keepdims=True))).astype(jnp.bfloat16)
    attended = jnp.einsum('rhcqk,rckhd->rcqhd', weights.astype(jnp.float32), value_blocks)
    return attended.astype(jnp.bfloat16).reshape(rows_n, GRID_W, heads_n, head_size)

def reference(hidden_in, norm_gain, query_weight, key_weight, value_weight, output_weight, offset_bias):
    all_rows = hidden_in.shape[0] // GRID_W
    span_half = ROW_SPAN // 2
    channels = HEADS * HEAD_DIM
    stream = hidden_in
    for layer_idx in range(LAYERS):
        stream_wide = stream.astype(jnp.float32)
        row_scale = lax.rsqrt(lax.optimization_barrier(jnp.mean(stream_wide * stream_wide, axis=1, keepdims=True)) + EPS)
        normed = (stream_wide * row_scale * norm_gain[layer_idx][None, :]).astype(jnp.bfloat16)
        query_grid = jnp.dot(normed, query_weight[layer_idx].T, preferred_element_type=jnp.float32).astype(jnp.bfloat16)
        key_grid = jnp.dot(normed, key_weight[layer_idx].T, preferred_element_type=jnp.float32).astype(jnp.bfloat16)
        value_grid = jnp.dot(normed, value_weight[layer_idx].T, preferred_element_type=jnp.float32).astype(jnp.bfloat16)
        query_grid = query_grid.reshape(all_rows, GRID_W, HEADS, HEAD_DIM)
        key_grid = key_grid.reshape(all_rows, GRID_W, HEADS, HEAD_DIM)
        value_grid = value_grid.reshape(all_rows, GRID_W, HEADS, HEAD_DIM)
        bias_table = offset_bias[layer_idx]

        def one_row(row_idx):
            first_row = jnp.clip(row_idx - span_half, 0, all_rows - ROW_SPAN).astype(jnp.int32)
            key_rows = lax.dynamic_slice_in_dim(key_grid, first_row, ROW_SPAN, 0)[None]
            value_rows = lax.dynamic_slice_in_dim(value_grid, first_row, ROW_SPAN, 0)[None]
            query_row = lax.dynamic_slice_in_dim(query_grid, row_idx, 1, 0)
            row_offset = (first_row + jnp.arange(ROW_SPAN, dtype=jnp.int32) - row_idx + ROW_SPAN - 1).astype(jnp.int32)[None]
            bias = bias_rows(bias_table, row_offset)
            return attend_rows(query_row, key_rows, value_rows, bias)[0]
        attended = lax.map(one_row, jnp.arange(all_rows, dtype=jnp.int32)).reshape(all_rows * GRID_W, channels)
        projected = jnp.dot(attended, output_weight[layer_idx], preferred_element_type=jnp.float32)
        stream = (stream.astype(jnp.float32) + projected).astype(jnp.bfloat16)
    return stream
```

```python
import functools

import jax
import jax.numpy as jnp
from jax import lax
from jax.experimental import pallas as pl
from jax.experimental.pallas import tpu as pltpu
from jax.sharding import PartitionSpec as P

HEAD_DIM = 64
GRID_W = 64
ROW_SPAN = 8
COL_SPAN = 16
EPS = 1e-06
NEG = -1e30
CHUNK_ROWS = 2
NT = (((1,), (1,)), ((), ()))


def kernel(
    n_tp, n_sp, hidden, gain, wq, wk, wv, wo, table, out,
    xbuf, att, kv, qbuf, normed, bias, wqkv, wout,
    w_sem, io_sem, xs, xr, xfs, xfr, ats, atr, afs, afr, hs, hr,
):
    layers = wqkv.shape[0]
    tokens, width = hidden.shape
    channels = qbuf.shape[1]
    features = n_tp * width
    rows_dev = tokens // GRID_W
    half = ROW_SPAN // 2
    halo = half * GRID_W
    chunk = CHUNK_ROWS * GRID_W
    chunks = tokens // chunk
    heads = channels // HEAD_DIM
    per_group = 2 if heads % 2 == 0 else 1
    groups = heads // per_group
    lanes = per_group * HEAD_DIM
    span = ROW_SPAN * GRID_W

    sp = lax.axis_index("sp")
    me = lax.axis_index("tp")
    core = lax.rem(me, 2)
    chip = me // 2
    chips = n_tp // 2
    sibling = me + 1 - 2 * core
    all_rows = rows_dev * n_sp
    first_row = sp * rows_dev

    def target(i):
        return lax.rem(chip + i, chips) * 2 + core

    def origin(i):
        return lax.rem(chip - i + chips, chips) * 2 + core

    own_copies = [
        pltpu.make_async_copy(
            hidden.at[pl.ds(c * chunk, chunk)],
            xbuf.at[0, me, pl.ds(c * chunk, chunk)],
            io_sem.at[c],
        )
        for c in range(chunks)
    ]
    for copy in own_copies:
        copy.start()

    def weight_copies(l):
        parts = [
            pltpu.make_async_copy(w.at[l], wqkv.at[l, pl.ds(i * channels, channels)], w_sem.at[l, i])
            for i, w in enumerate((wk, wv, wq))
        ]
        return parts, pltpu.make_async_copy(wo.at[l], wout.at[l], w_sem.at[l, 3])

    for l in range(layers):
        parts, last = weight_copies(l)
        for copy in parts:
            copy.start()
        last.start()

    barrier = pltpu.get_barrier_semaphore()
    for i in range(1, chips):
        pl.semaphore_signal(barrier, inc=1, device_id={"tp": target(i)})
    pl.semaphore_signal(barrier, inc=1, device_id={"tp": sibling})

    @pl.when(sp > 0)
    def _():
        pl.semaphore_signal(barrier, inc=1, device_id={"sp": sp - 1})

    @pl.when(sp < n_sp - 1)
    def _():
        pl.semaphore_signal(barrier, inc=1, device_id={"sp": sp + 1})

    pl.semaphore_wait(barrier, chips + jnp.minimum(sp, 1) + jnp.minimum(n_sp - 1 - sp, 1))

    def remote(buf, l, who, c, send, recv, i, dest):
        part = buf.at[l, who, pl.ds(c * chunk, chunk)]
        return pltpu.make_async_remote_copy(
            src_ref=part,
            dst_ref=part,
            send_sem=send.at[l, c, i],
            recv_sem=recv.at[l, c, i],
            device_id={"tp": dest},
        )

    def spread(buf, l, c, sems):
        for i in range(1, chips):
            remote(buf, l, me, c, sems[0], sems[1], i, target(i)).start()
        remote(buf, l, me, c, sems[0], sems[1], 0, sibling).start()

    def forward(buf, l, c, sems):
        for i in range(1, chips):
            remote(buf, l, origin(i), c, sems[0], sems[1], i, target(i)).wait_recv()
            remote(buf, l, origin(i), c, sems[2], sems[3], i, sibling).start()

    def collect(buf, l, c, sems):
        remote(buf, l, me, c, sems[0], sems[1], 0, sibling).wait_recv()
        for i in range(1, chips):
            remote(buf, l, origin(i), c, sems[2], sems[3], i, sibling).wait_recv()

    def drain(buf, l, c, sems):
        for i in range(chips):
            remote(buf, l, me, c, sems[0], sems[1], i, sibling).wait_send()
        for i in range(1, chips):
            remote(buf, l, me, c, sems[2], sems[3], i, sibling).wait_send()

    x_sems = (xs, xr, xfs, xfr)
    a_sems = (ats, atr, afs, afr)

    def up_copy(l, c):
        low = max(c * chunk, tokens - halo)
        size = (c + 1) * chunk - low
        if size <= 0:
            return None
        return pltpu.make_async_remote_copy(
            src_ref=kv.at[l, :, pl.ds(halo + low, size)],
            dst_ref=kv.at[l, :, pl.ds(low - (tokens - halo), size)],
            send_sem=hs.at[l, c, 0],
            recv_sem=hr.at[l, c, 0],
            device_id={"sp": sp + 1},
        )

    def down_copy(l, c):
        size = min((c + 1) * chunk, halo) - c * chunk
        if size <= 0:
            return None
        return pltpu.make_async_remote_copy(
            src_ref=kv.at[l, :, pl.ds(halo + c * chunk, size)],
            dst_ref=kv.at[l, :, pl.ds(halo + tokens + c * chunk, size)],
            send_sem=hs.at[l, c, 1],
            recv_sem=hr.at[l, c, 1],
            device_id={"sp": sp - 1},
        )

    def when_copy(condition, make, l, c, action):
        copy = make(l, c)
        if copy is None:
            return

        @pl.when(condition)
        def _():
            getattr(copy, action)()

    has_low = sp > 0
    has_high = sp < n_sp - 1

    for c in range(chunks):
        own_copies[c].wait()
        spread(xbuf, 0, c, x_sems)

    q_at = lax.broadcasted_iota(jnp.int32, (GRID_W, 2 * GRID_W), 0)
    k_at = lax.rem(lax.broadcasted_iota(jnp.int32, (GRID_W, 2 * GRID_W), 1), GRID_W)
    w_at = jnp.clip(q_at - COL_SPAN // 2, 0, GRID_W - COL_SPAN)
    inside = (k_at >= w_at) & (k_at < w_at + COL_SPAN)
    lane_low = lax.broadcasted_iota(jnp.int32, (GRID_W, lanes), 1) < HEAD_DIM

    def window_first(r):
        row = first_row + r
        return jnp.clip(row - half, 0, all_rows - ROW_SPAN)

    def make_bias(l):
        for r in range(rows_dev):
            j0 = window_first(r) - (first_row + r) + ROW_SPAN - 1
            for h in range(heads):
                for pair in range(ROW_SPAN // 2):
                    line = table[l, h, pl.ds(j0 + 2 * pair, 1), :]
                    rolled = pltpu.roll(
                        jnp.broadcast_to(line, (GRID_W, 2 * GRID_W)), 0, 1, stride=1, stride_axis=0
                    )
                    bias[
                        r,
                        h // per_group,
                        (h % per_group) * GRID_W : (h % per_group + 1) * GRID_W,
                        pair * 2 * GRID_W : (pair + 1) * 2 * GRID_W,
                    ] = jnp.where(inside, rolled, NEG)

    def project(l, c):
        rows = pl.ds(c * chunk, chunk)
        total = jnp.zeros((chunk, 1), jnp.float32)
        for t in range(n_tp):
            wide = xbuf[l, t, rows, :].astype(jnp.float32)
            total = total + jnp.sum(wide * wide, axis=1, keepdims=True)
        scale = lax.rsqrt(total * (1.0 / features) + EPS)
        for t in range(n_tp):
            cols = slice(t * width, (t + 1) * width)
            wide = xbuf[l, t, rows, :].astype(jnp.float32)
            gain_row = gain[0:1, cols]
            for k in range(1, layers):
                gain_row = jnp.where(l == k, gain[k : k + 1, cols], gain_row)
            normed[:, cols] = (wide * scale * gain_row).astype(jnp.bfloat16)
        made = [
            lax.dot_general(
                normed[...],
                wqkv[l, pl.ds(i * channels, channels), :],
                NT,
                preferred_element_type=jnp.float32,
            )
            for i in range(2)
        ]
        for i in range(2):
            kv[l, i, pl.ds(halo + c * chunk, chunk), :] = made[i].astype(jnp.bfloat16)
        when_copy(has_high, up_copy, l, c, "start")
        when_copy(has_low, down_copy, l, c, "start")
        queries = lax.dot_general(
            normed[...],
            wqkv[l, pl.ds(2 * channels, channels), :],
            NT,
            preferred_element_type=jnp.float32,
        )
        qbuf[rows, :] = (queries.astype(jnp.bfloat16) * HEAD_DIM**-0.5).astype(jnp.bfloat16)

    def attend(l, r):
        start = pl.multiple_of((window_first(r) - first_row + half) * GRID_W, GRID_W)
        rows = pl.ds(r * GRID_W, GRID_W)
        for g in range(groups):
            cols = slice(g * lanes, (g + 1) * lanes)
            query = qbuf[rows, cols]
            if per_group == 2:
                zero = jnp.zeros_like(query)
                query = jnp.concatenate(
                    [jnp.where(lane_low, query, zero), jnp.where(lane_low, zero, query)], axis=0
                )
            score = lax.dot_general(
                query, kv[l, 0, pl.ds(start, span), cols], NT, preferred_element_type=jnp.float32
            )
            score = score + bias[r, g]
            lifted = jnp.exp(score - jnp.max(score, axis=-1, keepdims=True))
            weights = lifted * (1.0 / jnp.sum(lifted, axis=-1, keepdims=True))
            mixed = jnp.dot(
                weights.astype(jnp.bfloat16),
                kv[l, 1, pl.ds(start, span), cols],
                preferred_element_type=jnp.float32,
            )
            if per_group == 2:
                mixed = jnp.where(lane_low, mixed[:GRID_W], mixed[GRID_W:])
            att[l, me, rows, cols] = mixed.astype(jnp.bfloat16)

    def out_copy(c):
        rows = pl.ds(c * chunk, chunk)
        return pltpu.make_async_copy(xbuf.at[layers, me, rows], out.at[rows], io_sem.at[c])

    def layer(l, carry):
        make_bias(l)
        parts, last = weight_copies(l)
        for c in range(chunks):
            forward(xbuf, l, c, x_sems)
            collect(xbuf, l, c, x_sems)
            if c == 0:
                for copy in parts:
                    copy.wait()
            project(l, c)
        for c in range(chunks):
            when_copy(has_low, up_copy, l, c, "wait_recv")
            when_copy(has_high, down_copy, l, c, "wait_recv")
        for r in range(rows_dev):
            attend(l, r)
            if (r + 1) % CHUNK_ROWS == 0:
                spread(att, l, r // CHUNK_ROWS, a_sems)
        last.wait()
        for c in range(chunks):
            rows = pl.ds(c * chunk, chunk)
            forward(att, l, c, a_sems)
            collect(att, l, c, a_sems)
            total = xbuf[l, me, rows, :].astype(jnp.float32)
            for t in range(n_tp):
                total = total + jnp.dot(
                    att[l, t, rows, :],
                    wout[l, t * channels : (t + 1) * channels, :],
                    preferred_element_type=jnp.float32,
                )
            xbuf[l + 1, me, rows, :] = total.astype(jnp.bfloat16)

            @pl.when(l + 1 < layers)
            def _():
                spread(xbuf, l + 1, c, x_sems)

            @pl.when(l + 1 == layers)
            def _():
                out_copy(c).start()

        return carry

    lax.fori_loop(0, layers, layer, 0)

    def finish(l, carry):
        for c in range(chunks):
            drain(xbuf, l, c, x_sems)
            drain(att, l, c, a_sems)
            when_copy(has_high, up_copy, l, c, "wait_send")
            when_copy(has_low, down_copy, l, c, "wait_send")
        return carry

    lax.fori_loop(0, layers, finish, 0)
    for c in range(chunks):
        out_copy(c).wait()


def bias_lines(offset_bias):
    spread = COL_SPAN - 1
    after = jnp.pad(offset_bias[:, :, 1:], ((0, 0), (0, 0), (0, 1), (0, 0)))
    gap = jnp.zeros(offset_bias.shape[:3] + (GRID_W - 2 * spread - 1,), jnp.float32)
    return jnp.concatenate(
        [offset_bias[..., spread:], gap, after, gap, offset_bias[..., :spread]], axis=-1
    )


def solution(mesh):
    n_tp, n_sp = mesh.shape["tp"], mesh.shape["sp"]

    def body(hidden, gain, wq, wk, wv, wo, offset_bias):
        tokens, width = hidden.shape
        layers, channels, features = wq.shape
        heads = channels // HEAD_DIM
        per_group = 2 if heads % 2 == 0 else 1
        rows_dev = tokens // GRID_W
        chunks = rows_dev // CHUNK_ROWS
        chips = n_tp // 2
        halo = ROW_SPAN // 2 * GRID_W
        any_spec = pl.BlockSpec(memory_space=pl.ANY)
        vmem_spec = pl.BlockSpec(memory_space=pltpu.VMEM)
        bf16 = jnp.bfloat16
        hop = pltpu.SemaphoreType.DMA((layers, chunks, chips))
        return pl.pallas_call(
            functools.partial(kernel, n_tp, n_sp),
            out_shape=jax.ShapeDtypeStruct((tokens, width), bf16),
            in_specs=[any_spec, vmem_spec] + [any_spec] * 4 + [vmem_spec],
            out_specs=any_spec,
            scratch_shapes=[
                pltpu.VMEM((layers + 1, n_tp, tokens, width), bf16),
                pltpu.VMEM((layers, n_tp, tokens, channels), bf16),
                pltpu.VMEM((layers, 2, tokens + 2 * halo, channels), bf16),
                pltpu.VMEM((tokens, channels), bf16),
                pltpu.VMEM((CHUNK_ROWS * GRID_W, features), bf16),
                pltpu.VMEM(
                    (rows_dev, heads // per_group, per_group * GRID_W, ROW_SPAN * GRID_W),
                    jnp.float32,
                ),
                pltpu.VMEM((layers, 3 * channels, features), bf16),
                pltpu.VMEM((layers, n_tp * channels, width), bf16),
                pltpu.SemaphoreType.DMA((layers, 4)),
                pltpu.SemaphoreType.DMA((chunks,)),
            ]
            + [hop] * 8
            + [pltpu.SemaphoreType.DMA((layers, chunks, 2))] * 2,
            compiler_params=pltpu.CompilerParams(
                collective_id=0, has_side_effects=True, vmem_limit_bytes=60 * 2**20
            ),
        )(hidden, gain, wq, wk, wv, wo, bias_lines(offset_bias))

    return jax.shard_map(
        body,
        mesh=mesh,
        in_specs=(
            P(("grp", "sp"), "tp"),
            P(),
            P(None, "tp", None),
            P(None, "tp", None),
            P(None, "tp", None),
            P(None, None, "tp"),
            P(None, "tp", None, None),
        ),
        out_specs=P(("grp", "sp"), "tp"),
        check_vma=False,
    )
```

```python
import functools

import jax
import jax.numpy as jnp
from jax import lax
from jax.experimental import pallas as pl
from jax.experimental.pallas import tpu as pltpu
from jax.sharding import PartitionSpec as P

HEAD_DIM = 64
GRID_W = 64
ROW_SPAN = 8
COL_SPAN = 16
EPS = 1e-06
NEG = -1e30
CHUNK_ROWS = 1
NT = (((1,), (1,)), ((), ()))


def kernel(
    n_tp, n_sp, hidden, gain, wq, wk, wv, wo, table, out,
    xbuf, att, kv, qbuf, scaled, squares, kv_sum, q_sum, out_sum, lines, bias, wqkv, wout,
    w_sem, io_sem, xs, xr, xfs, xfr, ats, atr, afs, afr, hs, hr,
):
    layers = wqkv.shape[0]
    tokens, width = hidden.shape
    channels = qbuf.shape[1]
    features = n_tp * width
    rows_dev = tokens // GRID_W
    half = ROW_SPAN // 2
    halo = half * GRID_W
    chunk = CHUNK_ROWS * GRID_W
    chunks = tokens // chunk
    heads = channels // HEAD_DIM
    per_group = 2 if heads % 2 == 0 else 1
    groups = heads // per_group
    lanes = per_group * HEAD_DIM
    span = ROW_SPAN * GRID_W

    sp = lax.axis_index("sp")
    me = lax.axis_index("tp")
    core = lax.rem(me, 2)
    chip = me // 2
    chips = n_tp // 2
    sibling = me + 1 - 2 * core
    all_rows = rows_dev * n_sp
    first_row = sp * rows_dev

    def target(i):
        return lax.rem(chip + i, chips) * 2 + core

    def origin_chip(i):
        return lax.rem(chip - i + chips, chips)

    def origin(i):
        return origin_chip(i) * 2 + core

    own_copies = [
        pltpu.make_async_copy(
            hidden.at[pl.ds(c * chunk, chunk)],
            xbuf.at[0, me, pl.ds(c * chunk, chunk)],
            io_sem.at[c],
        )
        for c in range(chunks)
    ]
    for copy in own_copies:
        copy.start()

    def weight_copies(l):
        parts = [
            pltpu.make_async_copy(w.at[l], wqkv.at[l, pl.ds(i * channels, channels)], w_sem.at[l, i])
            for i, w in enumerate((wk, wv, wq))
        ]
        return parts, pltpu.make_async_copy(wo.at[l], wout.at[l], w_sem.at[l, 3])

    for l in range(layers):
        parts, last = weight_copies(l)
        for copy in parts:
            copy.start()
        last.start()

    barrier = pltpu.get_barrier_semaphore()
    for i in range(1, chips):
        pl.semaphore_signal(barrier, inc=1, device_id={"tp": target(i)})
    pl.semaphore_signal(barrier, inc=1, device_id={"tp": sibling})

    @pl.when(sp > 0)
    def _():
        pl.semaphore_signal(barrier, inc=1, device_id={"sp": sp - 1})

    @pl.when(sp < n_sp - 1)
    def _():
        pl.semaphore_signal(barrier, inc=1, device_id={"sp": sp + 1})

    pl.semaphore_wait(barrier, chips + jnp.minimum(sp, 1) + jnp.minimum(n_sp - 1 - sp, 1))

    def remote(buf, l, who, c, send, recv, i, dest):
        part = buf.at[l, who, pl.ds(c * chunk, chunk)]
        return pltpu.make_async_remote_copy(
            src_ref=part,
            dst_ref=part,
            send_sem=send.at[l, c, i],
            recv_sem=recv.at[l, c, i],
            device_id={"tp": dest},
        )

    def spread(buf, l, c, sems):
        for i in range(1, chips):
            remote(buf, l, me, c, sems[0], sems[1], i, target(i)).start()
        remote(buf, l, me, c, sems[0], sems[1], 0, sibling).start()

    def forward(buf, l, c, sems):
        for i in range(1, chips):
            remote(buf, l, origin(i), c, sems[0], sems[1], i, target(i)).wait_recv()
            remote(buf, l, origin(i), c, sems[2], sems[3], i, sibling).start()

    def collect_own(buf, l, sems):
        for c in range(chunks):
            remote(buf, l, me, c, sems[0], sems[1], 0, sibling).wait_recv()

    def collect(buf, l, c, sems):
        for i in range(1, chips):
            remote(buf, l, origin(i), c, sems[2], sems[3], i, sibling).wait_recv()

    def drain(buf, l, c, sems):
        for i in range(chips):
            remote(buf, l, me, c, sems[0], sems[1], i, sibling).wait_send()
        for i in range(1, chips):
            remote(buf, l, me, c, sems[2], sems[3], i, sibling).wait_send()

    x_sems = (xs, xr, xfs, xfr)
    a_sems = (ats, atr, afs, afr)

    def up_copy(l, c):
        low = max(c * chunk, tokens - halo)
        size = (c + 1) * chunk - low
        if size <= 0:
            return None
        return pltpu.make_async_remote_copy(
            src_ref=kv.at[l, :, pl.ds(halo + low, size)],
            dst_ref=kv.at[l, :, pl.ds(low - (tokens - halo), size)],
            send_sem=hs.at[l, c, 0],
            recv_sem=hr.at[l, c, 0],
            device_id={"sp": sp + 1},
        )

    def down_copy(l, c):
        size = min((c + 1) * chunk, halo) - c * chunk
        if size <= 0:
            return None
        return pltpu.make_async_remote_copy(
            src_ref=kv.at[l, :, pl.ds(halo + c * chunk, size)],
            dst_ref=kv.at[l, :, pl.ds(halo + tokens + c * chunk, size)],
            send_sem=hs.at[l, c, 1],
            recv_sem=hr.at[l, c, 1],
            device_id={"sp": sp - 1},
        )

    def when_copy(condition, make, l, c, action):
        copy = make(l, c)
        if copy is None:
            return

        @pl.when(condition)
        def _():
            getattr(copy, action)()

    has_low = sp > 0
    has_high = sp < n_sp - 1

    for c in range(chunks):
        own_copies[c].wait()
        spread(xbuf, 0, c, x_sems)

    q_at = lax.broadcasted_iota(jnp.int32, (GRID_W, 2 * GRID_W), 0)
    k_at = lax.rem(lax.broadcasted_iota(jnp.int32, (GRID_W, 2 * GRID_W), 1), GRID_W)
    w_at = jnp.clip(q_at - COL_SPAN // 2, 0, GRID_W - COL_SPAN)
    inside = (k_at >= w_at) & (k_at < w_at + COL_SPAN)
    lane_low = lax.broadcasted_iota(jnp.int32, (GRID_W, lanes), 1) < HEAD_DIM

    def window_first(r):
        row = first_row + r
        return jnp.clip(row - half, 0, all_rows - ROW_SPAN)

    def make_bias(l):
        lines[...] = jnp.zeros_like(lines)
        for j in range(2 * ROW_SPAN - 1):
            lines[j, :, : 2 * COL_SPAN - 1] = table[l, j]
        for j in range(2 * ROW_SPAN - 2):
            lines[j] = pltpu.roll(lines[j], 2 * GRID_W - COL_SPAN + 1, 1) + pltpu.roll(
                lines[j + 1], GRID_W - COL_SPAN + 1, 1
            )
        for r in range(rows_dev):
            j0 = window_first(r) - (first_row + r) + ROW_SPAN - 1
            for h in range(heads):
                for pair in range(ROW_SPAN // 2):
                    line = lines[j0 + 2 * pair, h : h + 1, :]
                    rolled = pltpu.roll(
                        jnp.broadcast_to(line, (GRID_W, 2 * GRID_W)), 0, 1, stride=1, stride_axis=0
                    )
                    bias[
                        r,
                        h // per_group,
                        (h % per_group) * GRID_W : (h % per_group + 1) * GRID_W,
                        pair * 2 * GRID_W : (pair + 1) * 2 * GRID_W,
                    ] = jnp.where(inside, rolled, NEG)

    def columns(i):
        return pl.ds(pl.multiple_of(origin_chip(i) * 2 * width, 2 * width), 2 * width)

    def prepare(l, i, rows):
        total = squares[rows, :] if i else jnp.zeros((tokens, 1), jnp.float32)
        for u in range(2):
            at = origin_chip(i) * 2 + u
            cols = pl.ds(pl.multiple_of(at * width, width), width)
            gain_row = gain[0:1, cols]
            for k in range(1, layers):
                gain_row = jnp.where(l == k, gain[k : k + 1, cols], gain_row)
            wide = xbuf[l, at, rows, :].astype(jnp.float32)
            total = total + jnp.sum(wide * wide, axis=1, keepdims=True)
            slot = (2 * i + u) * width
            scaled[rows, slot : slot + width] = (wide * gain_row).astype(jnp.bfloat16)
        squares[rows, :] = total

    def product(l, i, rows, first, count):
        return lax.dot_general(
            scaled[rows, 2 * i * width : 2 * (i + 1) * width],
            wqkv[l, pl.ds(first, count), columns(i)],
            NT,
            preferred_element_type=jnp.float32,
        )

    def project_own(l):
        rows = pl.ds(0, tokens)
        prepare(l, 0, rows)
        kv_sum[...] = product(l, 0, rows, 0, 2 * channels)
        q_sum[...] = product(l, 0, rows, 2 * channels, channels)

    def scale_of(rows):
        return lax.rsqrt(squares[rows, :] * (1.0 / features) + EPS)

    def project_kv(l, c):
        rows = pl.ds(c * chunk, chunk)
        total = kv_sum[rows, :]
        for i in range(1, chips):
            prepare(l, i, rows)
            total = total + product(l, i, rows, 0, 2 * channels)
        made = (total * scale_of(rows)).astype(jnp.bfloat16)
        for k in range(2):
            kv[l, k, pl.ds(halo + c * chunk, chunk), :] = made[:, k * channels : (k + 1) * channels]
        when_copy(has_high, up_copy, l, c, "start")
        when_copy(has_low, down_copy, l, c, "start")

    def project_q(l):
        rows = pl.ds(0, tokens)
        total = q_sum[...]
        for i in range(1, chips):
            total = total + product(l, i, rows, 2 * channels, channels)
        queries = (total * scale_of(rows)).astype(jnp.bfloat16)
        qbuf[...] = (queries * HEAD_DIM**-0.5).astype(jnp.bfloat16)

    def attend(l, r):
        start = pl.multiple_of((window_first(r) - first_row + half) * GRID_W, GRID_W)
        rows = pl.ds(r * GRID_W, GRID_W)
        for g in range(groups):
            cols = slice(g * lanes, (g + 1) * lanes)
            query = qbuf[rows, cols]
            if per_group == 2:
                zero = jnp.zeros_like(query)
                query = jnp.concatenate(
                    [jnp.where(lane_low, query, zero), jnp.where(lane_low, zero, query)], axis=0
                )
            score = lax.dot_general(
                query, kv[l, 0, pl.ds(start, span), cols], NT, preferred_element_type=jnp.float32
            )
            score = score + bias[r, g]
            lifted = jnp.exp(score - jnp.max(score, axis=-1, keepdims=True))
            share = 1.0 / jnp.sum(lifted, axis=-1, keepdims=True)
            mixed = share * jnp.dot(
                lifted.astype(jnp.bfloat16),
                kv[l, 1, pl.ds(start, span), cols],
                preferred_element_type=jnp.float32,
            )
            if per_group == 2:
                mixed = jnp.where(lane_low, mixed[:GRID_W], mixed[GRID_W:])
            att[l, me, rows, cols] = mixed.astype(jnp.bfloat16)

    def out_copy(c):
        rows = pl.ds(c * chunk, chunk)
        return pltpu.make_async_copy(xbuf.at[layers, me, rows], out.at[rows], io_sem.at[c])

    def project_out_own(l):
        total = xbuf[l, me].astype(jnp.float32)
        for u in range(2):
            total = total + out_part(l, chip * 2 + u, pl.ds(0, tokens))
        out_sum[...] = total

    def out_part(l, at, rows):
        return jnp.dot(
            att[l, at, rows, :],
            wout[l, pl.ds(pl.multiple_of(at * channels, channels), channels), :],
            preferred_element_type=jnp.float32,
        )

    def project_out(l, c):
        rows = pl.ds(c * chunk, chunk)
        total = out_sum[rows, :]
        for i in range(1, chips):
            for u in range(2):
                total = total + out_part(l, origin_chip(i) * 2 + u, rows)
        xbuf[l + 1, me, rows, :] = total.astype(jnp.bfloat16)

        @pl.when(l + 1 < layers)
        def _():
            spread(xbuf, l + 1, c, x_sems)

        @pl.when(l + 1 == layers)
        def _():
            out_copy(c).start()

    def arrive(buf, l, sems, use):
        for c in range(chunks + 1):
            if c < chunks:
                forward(buf, l, c, sems)
            if c > 0:
                collect(buf, l, c - 1, sems)
                use(l, c - 1)

    def layer(l, carry):
        make_bias(l)
        parts, last = weight_copies(l)
        for copy in parts:
            copy.wait()
        collect_own(xbuf, l, x_sems)
        project_own(l)
        arrive(xbuf, l, x_sems, project_kv)
        project_q(l)
        for c in range(chunks):
            when_copy(has_low, up_copy, l, c, "wait_recv")
            when_copy(has_high, down_copy, l, c, "wait_recv")
        for r in range(rows_dev):
            attend(l, r)
            if (r + 1) % CHUNK_ROWS == 0:
                spread(att, l, r // CHUNK_ROWS, a_sems)
        last.wait()
        collect_own(att, l, a_sems)
        project_out_own(l)
        arrive(att, l, a_sems, project_out)
        return carry

    lax.fori_loop(0, layers, layer, 0)

    def finish(l, carry):
        for c in range(chunks):
            drain(xbuf, l, c, x_sems)
            drain(att, l, c, a_sems)
            when_copy(has_high, up_copy, l, c, "wait_send")
            when_copy(has_low, down_copy, l, c, "wait_send")
        return carry

    lax.fori_loop(0, layers, finish, 0)
    for c in range(chunks):
        out_copy(c).wait()


def solution(mesh):
    n_tp, n_sp = mesh.shape["tp"], mesh.shape["sp"]

    def body(hidden, gain, wq, wk, wv, wo, offset_bias):
        tokens, width = hidden.shape
        layers, channels, features = wq.shape
        heads = channels // HEAD_DIM
        per_group = 2 if heads % 2 == 0 else 1
        rows_dev = tokens // GRID_W
        chunks = rows_dev // CHUNK_ROWS
        chips = n_tp // 2
        halo = ROW_SPAN // 2 * GRID_W
        any_spec = pl.BlockSpec(memory_space=pl.ANY)
        vmem_spec = pl.BlockSpec(memory_space=pltpu.VMEM)
        bf16 = jnp.bfloat16
        hop = pltpu.SemaphoreType.DMA((layers, chunks, chips))
        return pl.pallas_call(
            functools.partial(kernel, n_tp, n_sp),
            out_shape=jax.ShapeDtypeStruct((tokens, width), bf16),
            in_specs=[any_spec, vmem_spec] + [any_spec] * 4 + [vmem_spec],
            out_specs=any_spec,
            scratch_shapes=[
                pltpu.VMEM((layers + 1, n_tp, tokens, width), bf16),
                pltpu.VMEM((layers, n_tp, tokens, channels), bf16),
                pltpu.VMEM((layers, 2, tokens + 2 * halo, channels), bf16),
                pltpu.VMEM((tokens, channels), bf16),
                pltpu.VMEM((tokens, features), bf16),
                pltpu.VMEM((tokens, 1), jnp.float32),
                pltpu.VMEM((tokens, 2 * channels), jnp.float32),
                pltpu.VMEM((tokens, channels), jnp.float32),
                pltpu.VMEM((tokens, width), jnp.float32),
                pltpu.VMEM((2 * ROW_SPAN - 1, heads, 2 * GRID_W), jnp.float32),
                pltpu.VMEM(
                    (rows_dev, heads // per_group, per_group * GRID_W, ROW_SPAN * GRID_W),
                    jnp.float32,
                ),
                pltpu.VMEM((layers, 3 * channels, features), bf16),
                pltpu.VMEM((layers, n_tp * channels, width), bf16),
                pltpu.SemaphoreType.DMA((layers, 4)),
                pltpu.SemaphoreType.DMA((chunks,)),
            ]
            + [hop] * 8
            + [pltpu.SemaphoreType.DMA((layers, chunks, 2))] * 2,
            compiler_params=pltpu.CompilerParams(
                collective_id=0, has_side_effects=True, vmem_limit_bytes=60 * 2**20
            ),
        )(hidden, gain, wq, wk, wv, wo, jnp.transpose(offset_bias, (0, 2, 1, 3)))

    return jax.shard_map(
        body,
        mesh=mesh,
        in_specs=(
            P(("grp", "sp"), "tp"),
            P(),
            P(None, "tp", None),
            P(None, "tp", None),
            P(None, "tp", None),
            P(None, None, "tp"),
            P(None, "tp", None, None),
        ),
        out_specs=P(("grp", "sp"), "tp"),
        check_vma=False,
    )
```

```python
import functools

import jax
import jax.numpy as jnp
from jax import lax
from jax.experimental import pallas as pl
from jax.experimental.pallas import tpu as pltpu
from jax.sharding import PartitionSpec as P

HEAD_DIM = 64
GRID_W = 64
ROW_SPAN = 8
COL_SPAN = 16
EPS = 1e-06
NEG = -1e30
CHUNK_ROWS = 1
NT = (((1,), (1,)), ((), ()))


def kernel(
    n_tp, n_sp, hidden, gain, wq, wk, wv, wo, table, out,
    xbuf, att, kv, qbuf, scaled, squares, kv_sum, q_sum, out_sum, lines, bias, wqkv, wout,
    w_sem, io_sem, xs, xr, xfs, xfr, ats, atr, afs, afr, hs, hr,
):
    layers = wqkv.shape[0]
    tokens, width = hidden.shape
    channels = qbuf.shape[1]
    features = n_tp * width
    rows_dev = tokens // GRID_W
    half = ROW_SPAN // 2
    halo = half * GRID_W
    chunk = CHUNK_ROWS * GRID_W
    chunks = tokens // chunk
    heads = channels // HEAD_DIM
    per_group = 2 if heads % 2 == 0 else 1
    groups = heads // per_group
    lanes = per_group * HEAD_DIM
    span = ROW_SPAN * GRID_W

    sp = lax.axis_index("sp")
    me = lax.axis_index("tp")
    core = lax.rem(me, 2)
    chip = me // 2
    chips = n_tp // 2
    sibling = me + 1 - 2 * core
    all_rows = rows_dev * n_sp
    first_row = sp * rows_dev

    def target(i):
        return lax.rem(chip + i, chips) * 2 + core

    def origin_chip(i):
        return lax.rem(chip - i + chips, chips)

    def origin(i):
        return origin_chip(i) * 2 + core

    own_copies = [
        pltpu.make_async_copy(
            hidden.at[pl.ds(c * chunk, chunk)],
            xbuf.at[0, me, pl.ds(c * chunk, chunk)],
            io_sem.at[c],
        )
        for c in range(chunks)
    ]
    for copy in own_copies:
        copy.start()

    def weight_copies(l):
        parts = [
            pltpu.make_async_copy(w.at[l], wqkv.at[l, pl.ds(i * channels, channels)], w_sem.at[l, i])
            for i, w in enumerate((wk, wv, wq))
        ]
        return parts, pltpu.make_async_copy(wo.at[l], wout.at[l], w_sem.at[l, 3])

    def fetch_weights(l):
        parts, last = weight_copies(l)
        for copy in parts:
            copy.start()
        last.start()

    fetch_weights(0)

    barrier = pltpu.get_barrier_semaphore()
    for i in range(1, chips):
        pl.semaphore_signal(barrier, inc=1, device_id={"tp": target(i)})
    pl.semaphore_signal(barrier, inc=1, device_id={"tp": sibling})

    @pl.when(sp > 0)
    def _():
        pl.semaphore_signal(barrier, inc=1, device_id={"sp": sp - 1})

    @pl.when(sp < n_sp - 1)
    def _():
        pl.semaphore_signal(barrier, inc=1, device_id={"sp": sp + 1})

    pl.semaphore_wait(barrier, chips + jnp.minimum(sp, 1) + jnp.minimum(n_sp - 1 - sp, 1))

    def remote(buf, l, who, c, send, recv, i, dest):
        part = buf.at[l, who, pl.ds(c * chunk, chunk)]
        return pltpu.make_async_remote_copy(
            src_ref=part,
            dst_ref=part,
            send_sem=send.at[l, c, i],
            recv_sem=recv.at[l, c, i],
            device_id={"tp": dest},
        )

    def spread(buf, l, c, sems):
        for i in range(1, chips):
            remote(buf, l, me, c, sems[0], sems[1], i, target(i)).start()
        remote(buf, l, me, c, sems[0], sems[1], 0, sibling).start()

    def forward(buf, l, c, sems):
        for i in range(1, chips):
            remote(buf, l, origin(i), c, sems[0], sems[1], i, target(i)).wait_recv()
            remote(buf, l, origin(i), c, sems[2], sems[3], i, sibling).start()

    def collect_own(buf, l, sems):
        for c in range(chunks):
            remote(buf, l, me, c, sems[0], sems[1], 0, sibling).wait_recv()

    def collect(buf, l, c, sems):
        for i in range(1, chips):
            remote(buf, l, origin(i), c, sems[2], sems[3], i, sibling).wait_recv()

    def drain(buf, l, c, sems):
        for i in range(chips):
            remote(buf, l, me, c, sems[0], sems[1], i, sibling).wait_send()
        for i in range(1, chips):
            remote(buf, l, me, c, sems[2], sems[3], i, sibling).wait_send()

    x_sems = (xs, xr, xfs, xfr)
    a_sems = (ats, atr, afs, afr)

    def up_copy(l, c):
        low = max(c * chunk, tokens - halo)
        size = (c + 1) * chunk - low
        if size <= 0:
            return None
        return pltpu.make_async_remote_copy(
            src_ref=kv.at[l, :, pl.ds(halo + low, size)],
            dst_ref=kv.at[l, :, pl.ds(low - (tokens - halo), size)],
            send_sem=hs.at[l, c, 0],
            recv_sem=hr.at[l, c, 0],
            device_id={"sp": sp + 1},
        )

    def down_copy(l, c):
        size = min((c + 1) * chunk, halo) - c * chunk
        if size <= 0:
            return None
        return pltpu.make_async_remote_copy(
            src_ref=kv.at[l, :, pl.ds(halo + c * chunk, size)],
            dst_ref=kv.at[l, :, pl.ds(halo + tokens + c * chunk, size)],
            send_sem=hs.at[l, c, 1],
            recv_sem=hr.at[l, c, 1],
            device_id={"sp": sp - 1},
        )

    def when_copy(condition, make, l, c, action):
        copy = make(l, c)
        if copy is None:
            return

        @pl.when(condition)
        def _():
            getattr(copy, action)()

    has_low = sp > 0
    has_high = sp < n_sp - 1

    def down_used(sender, c):
        return sender == 1 if c * chunk >= halo - GRID_W else sender > 0

    for c in range(chunks):
        own_copies[c].wait()
        spread(xbuf, 0, c, x_sems)

    q_at = lax.broadcasted_iota(jnp.int32, (GRID_W, 2 * GRID_W), 0)
    k_at = lax.rem(lax.broadcasted_iota(jnp.int32, (GRID_W, 2 * GRID_W), 1), GRID_W)
    w_at = jnp.clip(q_at - COL_SPAN // 2, 0, GRID_W - COL_SPAN)
    inside = (k_at >= w_at) & (k_at < w_at + COL_SPAN)
    lane_low = lax.broadcasted_iota(jnp.int32, (GRID_W, lanes), 1) < HEAD_DIM

    def window_first(r):
        row = first_row + r
        return jnp.clip(row - half, 0, all_rows - ROW_SPAN)

    def make_bias(l):
        lines[...] = jnp.zeros_like(lines)
        for j in range(2 * ROW_SPAN - 1):
            lines[j, :, : 2 * COL_SPAN - 1] = table[l, j]
        for j in range(2 * ROW_SPAN - 2):
            lines[j] = pltpu.roll(lines[j], 2 * GRID_W - COL_SPAN + 1, 1) + pltpu.roll(
                lines[j + 1], GRID_W - COL_SPAN + 1, 1
            )
        for r in range(rows_dev):
            j0 = window_first(r) - (first_row + r) + ROW_SPAN - 1
            for h in range(heads):
                for pair in range(ROW_SPAN // 2):
                    line = lines[j0 + 2 * pair, h : h + 1, :]
                    rolled = pltpu.roll(
                        jnp.broadcast_to(line, (GRID_W, 2 * GRID_W)), 0, 1, stride=1, stride_axis=0
                    )
                    bias[
                        r,
                        h // per_group,
                        (h % per_group) * GRID_W : (h % per_group + 1) * GRID_W,
                        pair * 2 * GRID_W : (pair + 1) * 2 * GRID_W,
                    ] = jnp.where(inside, rolled, NEG)

    def columns(i):
        return pl.ds(pl.multiple_of(origin_chip(i) * 2 * width, 2 * width), 2 * width)

    def prepare(l, i, rows):
        total = squares[rows, :] if i else jnp.zeros((tokens, 1), jnp.float32)
        for u in range(2):
            at = origin_chip(i) * 2 + u
            cols = pl.ds(pl.multiple_of(at * width, width), width)
            gain_row = gain[0:1, cols]
            for k in range(1, layers):
                gain_row = jnp.where(l == k, gain[k : k + 1, cols], gain_row)
            wide = xbuf[l, at, rows, :].astype(jnp.float32)
            total = total + jnp.sum(wide * wide, axis=1, keepdims=True)
            slot = (2 * i + u) * width
            scaled[rows, slot : slot + width] = (wide * gain_row).astype(jnp.bfloat16)
        squares[rows, :] = total

    def product(l, i, rows, first, count):
        return lax.dot_general(
            scaled[rows, 2 * i * width : 2 * (i + 1) * width],
            wqkv[l, pl.ds(first, count), columns(i)],
            NT,
            preferred_element_type=jnp.float32,
        )

    def project_own(l):
        rows = pl.ds(0, tokens)
        prepare(l, 0, rows)
        kv_sum[...] = product(l, 0, rows, 0, 2 * channels)
        q_sum[...] = product(l, 0, rows, 2 * channels, channels)

    def scale_of(rows):
        return lax.rsqrt(squares[rows, :] * (1.0 / features) + EPS)

    def project_kv(l, c):
        rows = pl.ds(c * chunk, chunk)
        total = kv_sum[rows, :]
        for i in range(1, chips):
            prepare(l, i, rows)
            total = total + product(l, i, rows, 0, 2 * channels)
        made = (total * scale_of(rows)).astype(jnp.bfloat16)
        for k in range(2):
            kv[l, k, pl.ds(halo + c * chunk, chunk), :] = made[:, k * channels : (k + 1) * channels]
        when_copy(has_high, up_copy, l, c, "start")
        when_copy(down_used(sp, c), down_copy, l, c, "start")

    def project_q(l):
        rows = pl.ds(0, tokens)
        total = q_sum[...]
        for i in range(1, chips):
            total = total + product(l, i, rows, 2 * channels, channels)
        queries = (total * scale_of(rows)).astype(jnp.bfloat16)
        qbuf[...] = (queries * HEAD_DIM**-0.5).astype(jnp.bfloat16)

    def attend(l, r):
        start = pl.multiple_of((window_first(r) - first_row + half) * GRID_W, GRID_W)
        rows = pl.ds(r * GRID_W, GRID_W)
        for g in range(groups):
            cols = slice(g * lanes, (g + 1) * lanes)
            query = qbuf[rows, cols]
            if per_group == 2:
                zero = jnp.zeros_like(query)
                query = jnp.concatenate(
                    [jnp.where(lane_low, query, zero), jnp.where(lane_low, zero, query)], axis=0
                )
            score = lax.dot_general(
                query, kv[l, 0, pl.ds(start, span), cols], NT, preferred_element_type=jnp.float32
            )
            score = score + bias[r, g]
            lifted = jnp.exp(score - jnp.max(score, axis=-1, keepdims=True))
            share = 1.0 / jnp.sum(lifted, axis=-1, keepdims=True)
            mixed = share * jnp.dot(
                lifted.astype(jnp.bfloat16),
                kv[l, 1, pl.ds(start, span), cols],
                preferred_element_type=jnp.float32,
            )
            if per_group == 2:
                mixed = jnp.where(lane_low, mixed[:GRID_W], mixed[GRID_W:])
            att[l, me, rows, cols] = mixed.astype(jnp.bfloat16)

    def out_copy(c):
        rows = pl.ds(c * chunk, chunk)
        return pltpu.make_async_copy(xbuf.at[layers, me, rows], out.at[rows], io_sem.at[c])

    def project_out_own(l):
        total = xbuf[l, me].astype(jnp.float32)
        for u in range(2):
            total = total + out_part(l, chip * 2 + u, pl.ds(0, tokens))
        out_sum[...] = total

    def out_part(l, at, rows):
        return jnp.dot(
            att[l, at, rows, :],
            wout[l, pl.ds(pl.multiple_of(at * channels, channels), channels), :],
            preferred_element_type=jnp.float32,
        )

    def project_out(l, c):
        rows = pl.ds(c * chunk, chunk)
        total = out_sum[rows, :]
        for i in range(1, chips):
            for u in range(2):
                total = total + out_part(l, origin_chip(i) * 2 + u, rows)
        xbuf[l + 1, me, rows, :] = total.astype(jnp.bfloat16)

        @pl.when(l + 1 < layers)
        def _():
            spread(xbuf, l + 1, c, x_sems)

        @pl.when(l + 1 == layers)
        def _():
            out_copy(c).start()

    def arrive(buf, l, sems, use):
        for c in range(chunks + 1):
            if c < chunks:
                forward(buf, l, c, sems)
            if c > 0:
                collect(buf, l, c - 1, sems)
                use(l, c - 1)

    def layer(l, carry):
        make_bias(l)
        parts, last = weight_copies(l)
        for copy in parts:
            copy.wait()

        @pl.when(l + 1 < layers)
        def _():
            fetch_weights(l + 1)

        collect_own(xbuf, l, x_sems)
        project_own(l)
        arrive(xbuf, l, x_sems, project_kv)
        project_q(l)
        for c in range(chunks):
            when_copy(has_low, up_copy, l, c, "wait_recv")
            when_copy(down_used(sp + 1, c) & has_high, down_copy, l, c, "wait_recv")
        for r in range(rows_dev):
            attend(l, r)
            if (r + 1) % CHUNK_ROWS == 0:
                spread(att, l, r // CHUNK_ROWS, a_sems)
        last.wait()
        collect_own(att, l, a_sems)
        project_out_own(l)
        arrive(att, l, a_sems, project_out)
        return carry

    lax.fori_loop(0, layers, layer, 0)

    def finish(l, carry):
        for c in range(chunks):
            drain(xbuf, l, c, x_sems)
            drain(att, l, c, a_sems)
            when_copy(has_high, up_copy, l, c, "wait_send")
            when_copy(down_used(sp, c), down_copy, l, c, "wait_send")
        return carry

    lax.fori_loop(0, layers, finish, 0)
    for c in range(chunks):
        out_copy(c).wait()


def solution(mesh):
    n_tp, n_sp = mesh.shape["tp"], mesh.shape["sp"]

    def body(hidden, gain, wq, wk, wv, wo, offset_bias):
        tokens, width = hidden.shape
        layers, channels, features = wq.shape
        heads = channels // HEAD_DIM
        per_group = 2 if heads % 2 == 0 else 1
        rows_dev = tokens // GRID_W
        chunks = rows_dev // CHUNK_ROWS
        chips = n_tp // 2
        halo = ROW_SPAN // 2 * GRID_W
        any_spec = pl.BlockSpec(memory_space=pl.ANY)
        vmem_spec = pl.BlockSpec(memory_space=pltpu.VMEM)
        bf16 = jnp.bfloat16
        hop = pltpu.SemaphoreType.DMA((layers, chunks, chips))
        return pl.pallas_call(
            functools.partial(kernel, n_tp, n_sp),
            out_shape=jax.ShapeDtypeStruct((tokens, width), bf16),
            in_specs=[any_spec, vmem_spec] + [any_spec] * 4 + [vmem_spec],
            out_specs=any_spec,
            scratch_shapes=[
                pltpu.VMEM((layers + 1, n_tp, tokens, width), bf16),
                pltpu.VMEM((layers, n_tp, tokens, channels), bf16),
                pltpu.VMEM((layers, 2, tokens + 2 * halo, channels), bf16),
                pltpu.VMEM((tokens, channels), bf16),
                pltpu.VMEM((tokens, features), bf16),
                pltpu.VMEM((tokens, 1), jnp.float32),
                pltpu.VMEM((tokens, 2 * channels), jnp.float32),
                pltpu.VMEM((tokens, channels), jnp.float32),
                pltpu.VMEM((tokens, width), jnp.float32),
                pltpu.VMEM((2 * ROW_SPAN - 1, heads, 2 * GRID_W), jnp.float32),
                pltpu.VMEM(
                    (rows_dev, heads // per_group, per_group * GRID_W, ROW_SPAN * GRID_W),
                    jnp.float32,
                ),
                pltpu.VMEM((layers, 3 * channels, features), bf16),
                pltpu.VMEM((layers, n_tp * channels, width), bf16),
                pltpu.SemaphoreType.DMA((layers, 4)),
                pltpu.SemaphoreType.DMA((chunks,)),
            ]
            + [hop] * 8
            + [pltpu.SemaphoreType.DMA((layers, chunks, 2))] * 2,
            compiler_params=pltpu.CompilerParams(
                collective_id=0, has_side_effects=True, vmem_limit_bytes=60 * 2**20
            ),
        )(hidden, gain, wq, wk, wv, wo, jnp.transpose(offset_bias, (0, 2, 1, 3)))

    return jax.shard_map(
        body,
        mesh=mesh,
        in_specs=(
            P(("grp", "sp"), "tp"),
            P(),
            P(None, "tp", None),
            P(None, "tp", None),
            P(None, "tp", None),
            P(None, None, "tp"),
            P(None, "tp", None, None),
        ),
        out_specs=P(("grp", "sp"), "tp"),
        check_vma=False,
    )
```
